128 devices in a mesh: ep: 128 (over z, y, x, core).
Axes of the slice: x: 4, y: 4, z: 4, core: 2. Of those that a mesh axis runs over, the one named last changes fastest.
Arguments:
- residual_in: bfloat16 [1024, 2048], P('ep'), may hold values from -6 to 6
- gain_mix_pre: float32 [2048], replicated, may hold values from 0.1 to 1.9
- w_query: bfloat16 [2048, 2048], P(None, 'ep'), may hold values from -0.125 to 0.125
- w_key: bfloat16 [2048, 2048], P(None, 'ep'), may hold values from -0.125 to 0.125
- w_value: bfloat16 [2048, 2048], P(None, 'ep'), may hold values from -0.125 to 0.125
- w_outgate: bfloat16 [2048, 2048], P(None, 'ep'), may hold values from -0.125 to 0.125
- w_decay: bfloat16 [2048, 16], replicated, may hold values from -0.125 to 0.125
- w_beta: bfloat16 [2048, 16], replicated, may hold values from -0.125 to 0.125
- decay_scale: float32 [16], replicated, may hold values from 1 to 16
- decay_bias: float32 [16], replicated, may hold values from -5 to -1
- head_gain: float32 [128], replicated, may hold values from 0.1 to 1.9
- w_out: bfloat16 [2048, 2048], replicated, may hold values from -0.125 to 0.125
- gain_mix_post: float32 [2048], replicated, may hold values from 0.1 to 1.9
- state_cache: bfloat16 [1024, 16, 128, 128], P('ep'), may hold values from -2.390625 to 2.390625
- gain_ffn_pre: float32 [2048], replicated, may hold values from 0.1 to 1.9
- routes: int32 [1024, 4], P('ep'), may hold values from 0 to 31, all different within a row; in each aligned block of 8 rows (0 to 7, 8 to 15, ...) at most 2 rows name the same one
- route_logits: float32 [1024, 4], P('ep'), may hold values from -6 to 6
- w_gate: bfloat16 [2048, 65536], P(None, 'ep'), may hold values from -0.375 to 0.375
- w_up: bfloat16 [2048, 65536], P(None, 'ep'), may hold values from -0.375 to 0.375
- w_down: bfloat16 [65536, 2048], P('ep'), may hold values from -0.125 to 0.125
- gain_ffn_post: float32 [2048], replicated, may hold values from 0.1 to 1.9
Outputs:
- result: bfloat16 [1024, 2048], P('ep')
- new_state: bfloat16 [1024, 16, 128, 128], P('ep')
The draws below stay inside these ranges and needn't reach their ends.
Inputs may be any that keep to these rules, and one draw needn't show every extreme that they name: `routes`: each row names 4 different experts. In the rows of one device (aligned blocks of 8 rows) no expert is named more than 2 times, and in some block one expert is named exactly 2 times.
All inputs are finite; a program needn't handle non-finite values.
Results may differ from the reference program's by a relative error of at most 0.014.
Values may be sent and summed in bfloat16 or wider, within the bound.
A program may use at most 128 MiB of HBM per device.

```python
import math
import jax
import jax.numpy as jnp
import numpy as np
from jax import lax

D = 2048
H = 16
HD = 128
FF = 2048
PIECES = 4
TOPK = 4
SEQ_DEV = 8
TOKENS = 1024
EXPERTS = 32
CAP = 2
N_EP = 128


def level_of(own_key, shape, shards, low, top_value):
    def one(position, blocks):
        steps = jax.random.uniform(jax.random.fold_in(jax.random.fold_in(own_key, 6), position), (blocks,), jnp.float32, low / len(shards), top_value / len(shards))
        return jnp.repeat(jnp.exp(steps), shape[position] // blocks).reshape((-1,) + (1,) * (len(shape) - position - 1))

    gain = one(*shards[0])
    for cut in shards[1:]:
        gain = gain * one(*cut)
    return gain


def deal_out(stream_key, own, number, rows, count, top, limit, lean):
    ranking = jax.random.permutation(stream_key, count)
    heavy_load, common = shares(count, rows * top, limit, lean, True), shares(count, rows * top, limit, lean, False)
    places = jnp.arange(count)

    def named(sizes, rotation):
        used = int((sizes > 0).sum())
        fixed = max(1, used // 4)
        moved = fixed + (places - fixed + rotation * (used - fixed)) % max(1, count - fixed)
        return jnp.zeros((count,), jnp.int32).at[ranking[jnp.where(places < fixed, places, moved)]].set(jnp.asarray(sizes, jnp.int32))

    sizes = jnp.where(number % 4 == 0, named(heavy_load, number // 4), named(common, number - number // 4 - 1))
    mixed = jax.random.permutation(jax.random.fold_in(own, 3), count)
    source_of, receiver = mixed[0:count // 2 * 2:2], mixed[1:count // 2 * 2:2]
    room = jnp.minimum(sizes[source_of] - 1, limit - sizes[receiver]) // 2
    room = jnp.where((source_of == ranking[0]) | (receiver == ranking[0]) | (sizes[receiver] == 0), 0, jnp.maximum(room, 0))
    moved = jax.random.randint(jax.random.fold_in(own, 4), (count // 2,), 0, 1 << 20) % (room + 1)
    sizes = sizes.at[source_of].add(-moved).at[receiver].add(moved)
    members = jnp.searchsorted(jnp.cumsum(sizes), jnp.arange(rows * top), side="right").astype(jnp.int32)
    table = members.reshape(top, rows).T
    table = table[jax.random.permutation(jax.random.fold_in(own, 1), rows)]
    rotation = jax.random.randint(jax.random.fold_in(own, 2), (rows, 1), 0, top)
    return jnp.take_along_axis(table, (jnp.arange(top)[None, :] + rotation) % top, axis=1)


def shares(number_of, total, bound, slope, full):
    loads = [(1 << 20) // math.isqrt(standing ** slope) + 1 for standing in range(1, number_of + 1)]
    largest = bound if full else min(bound, max(-(-total // number_of), total * loads[0] // sum(loads)))
    least = 1 if total - largest >= number_of - 1 else 0
    holding, rest = [largest] + [least] * (number_of - 1), total - largest - least * (number_of - 1)
    while rest > 0:
        free = [i for i in range(1, number_of) if holding[i] < largest] or [i for i in range(1, number_of) if holding[i] < bound]
        mass, remaining = sum([loads[i] for i in free]), rest
        for i in free:
            more = min(bound - holding[i], max(1, remaining * loads[i] // mass), rest)
            holding[i] = holding[i] + more
            rest = rest - more
    return np.array(holding)


def noise(key, shape, scale, limit, pieces=(), held_as=jnp.bfloat16):
    values = scale * jax.random.normal(key, shape, jnp.float32)
    if pieces:
        values = values * level_of(key, shape, pieces, -0.22, 0.18)
    return jnp.clip(values, -limit, limit).astype(held_as)


def setup_inputs(seed: int = 0) -> dict:
    key_of = jax.random.split(jax.random.key(seed), 22)
    residual_in = noise(key_of[0], (TOKENS, D), 1.0, 6.0, ((0, 128),))
    gain_mix_pre = jnp.clip(1.0 + 0.18 * jax.random.normal(key_of[1], (D,), jnp.float32), 0.1, 1.9)
    w_query = noise(key_of[2], (D, H * HD), D ** -0.5, 0.125, ((1, 128),))
    w_key = noise(key_of[3], (D, H * HD), D ** -0.5, 0.125, ((1, 128),))
    w_value = noise(key_of[4], (D, H * HD), D ** -0.5, 0.125, ((1, 128),))
    w_outgate = noise(key_of[5], (D, H * HD), D ** -0.5, 0.125, ((1, 128),))
    w_decay = noise(key_of[6], (D, H), D ** -0.5, 0.125)
    w_beta = noise(key_of[7], (D, H), D ** -0.5, 0.125)
    decay_scale = jnp.clip(jnp.exp(jax.random.uniform(key_of[8], (H,), jnp.float32, math.log(1.0), math.log(16.0))), 1.0, 16.0)
    decay_bias = jnp.clip(jax.random.uniform(key_of[9], (H,), jnp.float32, -5.0, -1.0), -5.0, -1.0)
    head_gain = jnp.clip(1.0 + 0.18 * jax.random.normal(key_of[10], (HD,), jnp.float32), 0.1, 1.9)
    w_out = noise(key_of[11], (H * HD, D), (H * HD) ** -0.5, 0.125)
    gain_mix_post = jnp.clip(1.0 + 0.18 * jax.random.normal(key_of[12], (D,), jnp.float32), 0.1, 1.9)
    state_cache = noise(key_of[13], (TOKENS, H, HD, HD), 0.3, 2.390625, ((0, 128),))
    gain_ffn_pre = jnp.clip(1.0 + 0.18 * jax.random.normal(key_of[14], (D,), jnp.float32), 0.1, 1.9)
    routes_keys = jax.random.split(jax.random.fold_in(key_of[15], 1), TOKENS // SEQ_DEV)
    routes_turns = jax.random.permutation(jax.random.fold_in(key_of[15], 3), TOKENS // SEQ_DEV)
    routes = jax.vmap(lambda own, number: deal_out(jax.random.fold_in(key_of[15], 2), own, number, SEQ_DEV, EXPERTS, TOPK, CAP, 1))(routes_keys, routes_turns).reshape((TOKENS, TOPK))
    route_logits = noise(key_of[16], (TOKENS, TOPK), 1.0, 6.0, ((0, 128),), jnp.float32)
    w_gate = noise(key_of[17], (D, EXPERTS * FF), (D // 9) ** -0.5, 0.375, ((1, 128),))
    w_up = noise(key_of[18], (D, EXPERTS * FF), (D // 9) ** -0.5, 0.375, ((1, 128),))
    w_down = noise(key_of[19], (EXPERTS * FF, D), FF ** -0.5, 0.125, ((0, 128),))
    gain_ffn_post = jnp.clip(1.0 + 0.18 * jax.random.normal(key_of[20], (D,), jnp.float32), 0.1, 1.9)
    return dict(residual_in=residual_in, gain_mix_pre=gain_mix_pre, w_query=w_query, w_key=w_key, w_value=w_value, w_outgate=w_outgate, w_decay=w_decay, w_beta=w_beta, decay_scale=decay_scale, decay_bias=decay_bias, head_gain=head_gain, w_out=w_out, gain_mix_post=gain_mix_post, state_cache=state_cache, gain_ffn_pre=gain_ffn_pre, routes=routes, route_logits=route_logits, w_gate=w_gate, w_up=w_up, w_down=w_down, gain_ffn_post=gain_ffn_post)


EPS = 1e-06
LIMIT = 7.0
ALPHA = 1.702

def rms_scale(values):
    return values * lax.rsqrt(lax.optimization_barrier(jnp.mean(values * values, axis=-1, keepdims=True)) + EPS)

def clamped_unit(gate, upper):
    glu = jnp.minimum(gate, LIMIT)
    linear = jnp.clip(upper, -LIMIT, LIMIT)
    return glu * jax.nn.sigmoid(ALPHA * glu) * (linear + 1.0)

def dispatch_table(routes, experts, capacity):
    count, topk = routes.shape
    hits = (routes[:, :, None] == jnp.arange(experts, dtype=jnp.int32)).astype(jnp.int32)
    flat = hits.reshape(count * topk, experts)
    before = jnp.cumsum(flat, axis=0) - flat
    slots = lax.optimization_barrier(jnp.sum(before * flat, axis=1)).reshape(count, topk)
    target = routes * capacity + slots
    return (target[:, :, None] == jnp.arange(experts * capacity, dtype=jnp.int32)).astype(jnp.float32)

def delta_step(q_raw, k_raw, v_raw, z_raw, decay_in, beta_in, state, decay_scale, decay_bias, head_gain):
    count = q_raw.shape[0]
    query = jax.nn.silu(q_raw.astype(jnp.float32)).reshape(count, H, HD)
    query = query * lax.rsqrt(lax.optimization_barrier(jnp.sum(query * query, axis=-1, keepdims=True)) + EPS) * HD ** (-0.5)
    keys = jax.nn.silu(k_raw.astype(jnp.float32)).reshape(count, H, HD)
    keys = keys * lax.rsqrt(lax.optimization_barrier(jnp.sum(keys * keys, axis=-1, keepdims=True)) + EPS)
    values = jax.nn.silu(v_raw.astype(jnp.float32)).reshape(count, H, HD)
    decay = -decay_scale * jax.nn.softplus(decay_in + decay_bias)
    beta = jax.nn.sigmoid(beta_in)
    held = state.astype(jnp.float32) * jnp.exp(decay)[:, :, None, None]
    guess = jnp.einsum('rhk,rhkv->rhv', keys, held)
    held = held + jnp.einsum('rhk,rhv->rhkv', keys, beta[:, :, None] * (values - guess))
    output = jnp.einsum('rhk,rhkv->rhv', query, held)
    output = rms_scale(output) * head_gain
    gated = output.reshape(count, H * HD) * jax.nn.silu(z_raw.astype(jnp.float32))
    return (gated.astype(jnp.bfloat16), held.astype(jnp.bfloat16))

def reference(residual_in, gain_mix_pre, w_query, w_key, w_value, w_outgate, w_decay, w_beta, decay_scale, decay_bias, head_gain, w_out, gain_mix_post, state_cache, gain_ffn_pre, routes, route_logits, w_gate, w_up, w_down, gain_ffn_post):
    x_first = residual_in.astype(jnp.float32)
    normed = (rms_scale(x_first) * gain_mix_pre).astype(jnp.bfloat16)

    def project(weight):
        return jnp.dot(normed, weight, preferred_element_type=jnp.float32).astype(jnp.bfloat16)
    q_raw, k_raw, v_raw, z_raw = (project(w_query), project(w_key), project(w_value), project(w_outgate))
    decay_in = jnp.dot(normed, w_decay, preferred_element_type=jnp.float32)
    beta_in = jnp.dot(normed, w_beta, preferred_element_type=jnp.float32)

    def blocks(array):
        return array.reshape((N_EP, SEQ_DEV) + array.shape[1:])

    def block_step(items):
        return delta_step(*items, decay_scale, decay_bias, head_gain)
    mixed, new_state = lax.map(block_step, tuple((blocks(a) for a in (q_raw, k_raw, v_raw, z_raw, decay_in, beta_in, state_cache))))
    mixed = mixed.reshape(TOKENS, H * HD)
    new_state = new_state.reshape(TOKENS, H, HD, HD)
    branch = jnp.dot(mixed, w_out, preferred_element_type=jnp.float32)
    x_second = x_first + rms_scale(branch) * gain_mix_post
    normed_two = (rms_scale(x_second) * gain_ffn_pre).astype(jnp.bfloat16)
    table = jax.vmap(lambda r: dispatch_table(r, EXPERTS, CAP))(routes.reshape(N_EP, SEQ_DEV, TOPK))
    picks = lax.optimization_barrier(jnp.sum(table, axis=2))
    sent = jnp.einsum('nse,nsd->ned', picks, normed_two.reshape(N_EP, SEQ_DEV, D).astype(jnp.float32), precision=lax.Precision.HIGHEST).astype(jnp.bfloat16)
    sent = sent.reshape(N_EP, EXPERTS, CAP, D).transpose(1, 0, 2, 3).reshape(EXPERTS, N_EP * CAP, D)
    width = FF // PIECES

    def expert(items):
        rows_in, index = items
        total = jnp.zeros((N_EP * CAP, D), jnp.float32)
        for part in range(PIECES):
            start = (index * FF + part * width).astype(jnp.int32)
            gate_cols = lax.dynamic_slice_in_dim(w_gate, start, width, 1)
            up_cols = lax.dynamic_slice_in_dim(w_up, start, width, 1)
            down_rows = lax.dynamic_slice_in_dim(w_down, start, width, 0)
            hidden = clamped_unit(jnp.dot(rows_in, gate_cols, preferred_element_type=jnp.float32), jnp.dot(rows_in, up_cols, preferred_element_type=jnp.float32)).astype(jnp.bfloat16)
            piece_out = jnp.dot(hidden, down_rows, preferred_element_type=jnp.float32).astype(jnp.bfloat16)
            piece_out = lax.optimization_barrier(piece_out)
            total = total + piece_out.astype(jnp.float32)
        return total
    outputs = lax.map(expert, (sent, jnp.arange(EXPERTS, dtype=jnp.int32)))
    outputs = outputs.reshape(EXPERTS, N_EP, CAP, D).transpose(1, 0, 2, 3).reshape(N_EP, EXPERTS * CAP, D)
    raised = jnp.exp(route_logits)
    weights = raised / lax.optimization_barrier(jnp.sum(raised, axis=-1, keepdims=True))
    mix_table = jnp.einsum('nske,nsk->nse', table, weights.reshape(N_EP, SEQ_DEV, TOPK))
    moe = jnp.einsum('nse,ned->nsd', mix_table, outputs, precision=lax.Precision.HIGHEST).reshape(TOKENS, D)
    result = (x_second + rms_scale(moe) * gain_ffn_post).astype(jnp.bfloat16)
    return (result, new_state)
```

```python
import jax
import jax.numpy as jnp
from jax import lax
from jax.experimental import pallas as pl
from jax.experimental.pallas import tpu as pltpu
from jax.sharding import PartitionSpec as P

H = 16
HD = 128
D = 2048
CHIPS = 64
EPS = 1e-06
LIMIT = 7.0
ALPHA = 1.702
BF = jnp.bfloat16
F32 = jnp.float32
MESH = pl.DeviceIdType.MESH


def rsqrt_mean(values):
    return lax.rsqrt(jnp.mean(values * values, axis=-1, keepdims=True) + EPS)


def silu(values):
    return values * jax.nn.sigmoid(values)


def nt_dot(a, b):
    return lax.dot_general(a, b, (((1,), (1,)), ((), ())), preferred_element_type=F32)


def tn_dot(a, b):
    return lax.dot_general(a, b, (((0,), (0,)), ((), ())), preferred_element_type=F32)


def dot(a, b):
    return jnp.dot(a, b, preferred_element_type=F32)


def iota(shape, dim):
    return lax.broadcasted_iota(jnp.int32, shape, dim)


COLS = ((0, 640), (640, 1280), (1280, 2048))
RING = (0, 2, 1)
PLANE = ((1, 2), (0, 1), (2, 0))
FAR_FIRST = sorted(
    [(dz, dy, dx) for dz in range(4) for dy in range(4) for dx in range(4) if dz + dy + dx],
    key=lambda d: -sum(min(v, 4 - v) for v in d),
)


def layer_kernel(
    x_ref,
    gain_pre,
    w_decay,
    w_beta,
    decay_scale,
    decay_bias,
    head_gain,
    gain_post,
    gain_ffn,
    routes,
    logits,
    gain_out,
    wq_hbm,
    wk_hbm,
    wv_hbm,
    wz_hbm,
    wout_hbm,
    state_hbm,
    gate_hbm,
    up_hbm,
    down_hbm,
    result_ref,
    nsbuf,
    wall,
    nbuf,
    pacc,
    pbuf,
    qbuf,
    qs,
    ks,
    vs,
    zs,
    egs,
    betas,
    kqs,
    mix_o,
    sbuf,
    wout,
    gate,
    up,
    down,
    branch,
    sent,
    xbuf,
    hbuf,
    part,
    rbuf,
    own_sem,
    w_send,
    w_recv,
    a_send,
    a_recv,
    b_send,
    b_recv,
    p_send,
    p_recv,
    d_send,
    d_recv,
    c_send,
    c_recv,
):
    me = lax.axis_index("ep")
    core = lax.rem(me, 2)
    chip = lax.div(me, 2)
    cx = lax.rem(chip, 4)
    cy = lax.rem(lax.div(chip, 4), 4)
    cz = lax.div(chip, 16)
    partner = chip * 2 + (1 - core)
    coords = (cz, cy, cx)
    ahead = [[c if d == 0 else lax.rem(c + d, 4) for d in range(4)] for c in coords]
    back = [[c if d == 0 else lax.rem(c + 4 - d, 4) for d in range(4)] for c in coords]
    zy = [[ahead[0][dz] * 32 + ahead[1][dy] * 8 + core for dy in range(4)] for dz in range(4)]
    x2 = [ahead[2][dx] * 2 for dx in range(4)]
    zy_slot = [[ahead[0][dz] * 32 + ahead[1][dy] * 8 for dy in range(4)] for dz in range(4)]
    zy_expert = [[ahead[0][dz] * 16 + ahead[1][dy] * 4 for dy in range(4)] for dz in range(4)]
    x_expert = [lax.div(ahead[2][dx], 2) * 2 for dx in range(4)]

    def device(d):
        return zy[d[0]][d[1]] + x2[d[2]]

    types = (wq_hbm, wk_hbm, wv_hbm, wz_hbm)
    fetches = []
    wall_rows = []
    for r, ref in enumerate(types):
        row = pl.multiple_of(lax.rem(cx + r, 4) * 32 + core * 16, 16)
        wall_rows.append(row)
        fetches.append(pltpu.make_async_copy(ref, wall.at[pl.ds(row, 16)], own_sem.at[r]))
    fetches.append(pltpu.make_async_copy(state_hbm, sbuf, own_sem.at[4]))
    fetches.append(pltpu.make_async_copy(wout_hbm, wout, own_sem.at[5]))
    fetches.append(pltpu.make_async_copy(gate_hbm, gate.at[:, 0:512], own_sem.at[6]))
    fetches.append(pltpu.make_async_copy(up_hbm, up.at[:, 0:512], own_sem.at[7]))
    fetches.append(pltpu.make_async_copy(down_hbm, down.at[0:512], own_sem.at[8]))
    for fetch in fetches:
        fetch.start()

    barrier = pltpu.get_barrier_semaphore()
    for d in FAR_FIRST:
        pl.semaphore_signal(barrier, inc=1, device_id=(device(d),), device_id_type=MESH)
    pl.semaphore_signal(barrier, inc=1, device_id=(partner,), device_id_type=MESH)

    x_first = x_ref[...].astype(F32)
    normed = (x_first * rsqrt_mean(x_first) * gain_pre[...]).astype(BF)
    nbuf[cz, cy, cx] = normed
    pacc[...] = jnp.zeros_like(pacc)
    decay_in = nt_dot(normed, w_decay[...])
    beta_in = nt_dot(normed, w_beta[...])

    pl.semaphore_wait(barrier, CHIPS)

    def swap(src, dst, k):
        return pltpu.make_async_remote_copy(
            src_ref=src,
            dst_ref=dst,
            send_sem=w_send.at[k],
            recv_sem=w_recv.at[k],
            device_id=(partner,),
            device_id_type=MESH,
        )

    swaps = [swap(ref, wall.at[pl.ds(wall_rows[r], 16)], r) for r, ref in enumerate(types)]
    swaps.append(swap(gate_hbm, gate.at[:, 512:1024], 4))
    swaps.append(swap(up_hbm, up.at[:, 512:1024], 5))
    swaps.append(swap(down_hbm, down.at[512:1024], 6))
    for s in swaps[:4]:
        s.start()

    def send(src, dst, send_sem, recv_sem, target):
        return pltpu.make_async_remote_copy(
            src_ref=src,
            dst_ref=dst,
            send_sem=send_sem,
            recv_sem=recv_sem,
            device_id=(target,),
            device_id_type=MESH,
        )

    def amount(ref, send_sem, recv_sem):
        return send(ref, ref, send_sem, recv_sem, partner)

    def offset(color, a, b, o):
        d = [0, 0, 0]
        d[PLANE[color][0]], d[PLANE[color][1]], d[RING[color]] = a, b, o
        return tuple(d)

    def columns_of(color):
        return slice(*COLS[color])

    for a in range(4):
        for b in range(4):
            for color in range(3):
                if a + b:
                    block = nbuf.at[cz, cy, cx, :, columns_of(color)]
                    to = device(offset(color, a, b, 0))
                    send(block, block, a_send.at[color], a_recv.at[color, a], to).start()
    for s in swaps[4:]:
        s.start()

    decay = jnp.exp(-decay_scale[...] * jax.nn.softplus(decay_in + decay_bias[...]))
    beta = jax.nn.sigmoid(beta_in)
    for h in range(H):
        egs[h] = jnp.broadcast_to(decay[:, h : h + 1], (8, HD))
        betas[h] = jnp.broadcast_to(beta[:, h : h + 1], (8, HD))

    def index_of(color, a, o):
        index = [slice(None)] * 3
        index[RING[color]] = back[RING[color]][o]
        if a is not None:
            index[PLANE[color][0]] = back[PLANE[color][0]][a]
        return tuple(index)

    for a in range(4):
        for color in range(3):
            cols = columns_of(color)
            arrived = nbuf.at[0, 0, 0 : 3 if a == 0 else 4, :, cols]
            amount(arrived, a_send.at[color], a_recv.at[color, a]).wait_recv()
            block = nbuf.at[index_of(color, a, 0) + (slice(None), cols)]
            for o in (2, 1, 3):
                to = device(offset(color, 0, 0, o))
                send(block, block, b_send.at[color], b_recv.at[color, o], to).start()

    for r in range(4):
        fetches[r].wait()
        swaps[r].wait_recv()
    for o in (0, 1, 3, 2):
        for color in range(3):
            cols = columns_of(color)
            if o:
                arrived = nbuf.at[0, :, :, :, cols]
                amount(arrived, b_send.at[color], b_recv.at[color, o]).wait_recv()
            where = index_of(color, None, o)
            rows = nbuf[where + (slice(None), cols)].reshape(128, -1)
            got = nt_dot(rows, wall[:, cols]).reshape(4, 4, 8, 128)
            pacc[where] += got
    pbuf[...] = pacc[...].astype(BF)
    for d in FAR_FIRST:
        src = pbuf.at[ahead[0][d[0]], ahead[1][d[1]], ahead[2][d[2]]]
        send(src, qbuf.at[cz, cy, cx], p_send, p_recv, device(d)).start()

    before_mask = (iota((8, 8), 0) < iota((8, 8), 1)).astype(BF)

    def hits_of(expert):
        return [(routes[j : j + 1, :] == expert).astype(F32) for j in range(4)]

    def earlier(hits):
        return dot(hits.astype(BF), before_mask)

    slot64 = lax.rem(iota((64, 8), 0), 2).astype(F32)
    hits64 = sum(hits_of(lax.div(iota((64, 8), 0), 2)))
    picks = jnp.where(earlier(hits64) == slot64, hits64, 0.0).astype(BF)
    row128 = iota((128, 8), 0)
    slot128 = lax.rem(row128, 2).astype(F32)
    own128 = lax.div(row128, 2) == chip
    hits_own = sum(hits_of(jnp.where(own128, lax.div(chip, 2), -1)))
    picks_own = jnp.where(earlier(hits_own) == slot128, hits_own, 0.0).astype(BF)
    raised = jnp.exp(logits[...])
    weights = raised / jnp.sum(raised, axis=0, keepdims=True)
    hits_each = hits_of(lax.div(row128, 4))
    weighed = sum(weights[j : j + 1, :] * hits_each[j] for j in range(4))
    mix = jnp.where(earlier(sum(hits_each)) == slot128, weighed, 0.0).T
    mix_hi = mix.astype(BF)
    mix_lo = (mix - mix_hi.astype(F32)).astype(BF)
    mix_both = jnp.concatenate([mix_hi, mix_lo], axis=0)

    fetches[4].wait()
    columns_in = wout.at[0:504, 0:128]
    amount(columns_in, p_send, p_recv).wait_recv()
    group = lax.div(iota((8, HD), 1), 32)
    seq = iota((8, HD), 0)
    for h in range(H):
        blocks = []
        for i in range(4):
            n = 4 * h + i
            at = (n // 16, n // 4 % 4, n % 4)
            blocks.append(jnp.where(n == chip, pbuf[at].astype(F32), qbuf[at].astype(F32)))
        heads = []
        for r in range(4):
            order = [blocks[(g - r) % 4] for g in range(4)]
            taken = jnp.where(
                group < 2,
                jnp.where(group == 0, order[0], order[1]),
                jnp.where(group == 2, order[2], order[3]),
            )
            heads.append(taken if r == 0 else pltpu.roll(taken, 128 - 32 * r, 1))
        query = silu(heads[0])
        query = query * lax.rsqrt(jnp.sum(query * query, -1, keepdims=True) + EPS) * HD ** (-0.5)
        keys = silu(heads[1])
        keys = keys * lax.rsqrt(jnp.sum(keys * keys, -1, keepdims=True) + EPS)
        qs[h] = query
        ks[h] = keys
        vs[h] = silu(heads[2])
        zs[h] = silu(heads[3])
        kqs[h] = jnp.broadcast_to(jnp.sum(query * keys, -1, keepdims=True), (8, HD))

    def head_step(step, carry):
        for i in range(4):
            h = step * 4 + i
            k, q, eg = ks[h], qs[h], egs[h]
            k_hi, q_hi = k.astype(BF).astype(F32), q.astype(BF).astype(F32)
            left = jnp.concatenate([k_hi, q_hi, k - k_hi, q - q_hi], axis=0).astype(BF)
            s_k = jnp.zeros((8, HD), F32)
            s_q = jnp.zeros((8, HD), F32)
            for s in range(8):
                got = dot(left, sbuf[s, h])
                s_k = jnp.where(seq == s, got[0:8] + got[16:24], s_k)
                s_q = jnp.where(seq == s, got[8:16] + got[24:32], s_q)
            update = betas[h] * (vs[h] - eg * s_k)
            out = eg * s_q + kqs[h] * update
            out = out * rsqrt_mean(out) * head_gain[...]
            mix_o[h] = out * zs[h]
            vs[h] = update
        return carry

    lax.fori_loop(0, 4, head_step, 0)

    fetches[5].wait()
    mixed = jnp.concatenate([mix_o[h] for h in range(H)], axis=1).astype(BF)

    def out_step(n, carry):
        cols = pl.ds(pl.multiple_of(n * 512, 512), 512)
        branch[:, cols] = dot(mixed, wout[:, cols])
        return carry

    lax.fori_loop(0, 4, out_step, 0)
    value = branch[...]
    x_second = x_ref[...].astype(F32) + value * rsqrt_mean(value) * gain_post[...]
    normed_two = (x_second * rsqrt_mean(x_second) * gain_ffn[...]).astype(BF)

    sent[...] = dot(picks, normed_two).astype(BF)
    own_slot = pl.ds(pl.multiple_of(chip * 2, 2), 2)
    for d in FAR_FIRST:
        src = sent.at[pl.ds(pl.multiple_of(zy_expert[d[0]][d[1]] + x_expert[d[2]], 2), 2)]
        send(src, xbuf.at[own_slot], d_send, d_recv, device(d)).start()
    own_sent = dot(picks_own, normed_two).astype(BF)

    seq16 = lax.rem(iota((16, HD), 0), 8)

    def state_step(step, carry):
        for i in range(2):
            h = step * 2 + i
            k, eg, update = ks[h], egs[h], vs[h]
            k_hi = k.astype(BF).astype(F32)
            columns = jnp.concatenate([k_hi, k - k_hi], axis=0).T.astype(BF)
            twice = jnp.concatenate([update, update], axis=0)
            for s in range(0, 8, 2):
                pair = jnp.concatenate(
                    [jnp.where(seq16 == s, twice, 0.0), jnp.where(seq16 == s + 1, twice, 0.0)],
                    axis=1,
                ).astype(BF)
                outer = dot(columns, pair)
                for t in range(2):
                    kept = sbuf[s + t, h].astype(F32) * eg[s + t : s + t + 1, :]
                    nsbuf[s + t, h] = (kept + outer[:, 128 * t : 128 * t + 128]).astype(BF)
        return carry

    lax.fori_loop(0, 8, state_step, 0)
    for k in range(6, 9):
        fetches[k].wait()
        swaps[k - 2].wait_recv()
    rows_in = wout.at[0:224, 0:1152]
    amount(rows_in, d_send, d_recv).wait_recv()
    own_row = lax.div(iota((128, D), 0), 2) == chip
    xbuf[...] = jnp.where(own_row, own_sent.astype(F32), xbuf[...].astype(F32)).astype(BF)

    def hidden_step(n, carry):
        cols = pl.ds(pl.multiple_of(n * 256, 256), 256)
        a = dot(xbuf[...], gate[:, cols])
        b = dot(xbuf[...], up[:, cols])
        m = jnp.minimum(a, LIMIT)
        unit = m * jax.nn.sigmoid(ALPHA * m) * (jnp.clip(b, -LIMIT, LIMIT) + 1.0)
        hbuf[:, cols] = unit.astype(BF)
        return carry

    lax.fori_loop(0, 4, hidden_step, 0)

    def down_step(n, carry):
        cols = pl.ds(pl.multiple_of(n * 1024, 1024), 1024)
        part[:, cols] = dot(hbuf[...], down[:, cols]).astype(BF)
        return carry

    lax.fori_loop(0, 2, down_step, 0)

    for d in FAR_FIRST:
        src = part.at[pl.ds(pl.multiple_of(zy_slot[d[0]][d[1]] + x2[d[2]], 2), 2)]
        send(src, rbuf.at[own_slot], c_send, c_recv, device(d)).start()
    amount(rows_in, c_send, c_recv).wait_recv()
    returned = jnp.where(own_row, part[...].astype(F32), rbuf[...].astype(F32)).astype(BF)
    moe = dot(mix_both, returned)
    moe = moe[0:8] + moe[8:16]
    result_ref[...] = (x_second + moe * rsqrt_mean(moe) * gain_out[...]).astype(BF)

    for s in swaps:
        s.wait_send()
    for color in range(3):
        cols = columns_of(color)
        amount(wout.at[0:120, cols], a_send.at[color], a_recv.at[color, 0]).wait_send()
        amount(nbuf.at[0:3, :, :, :, cols], b_send.at[color], b_recv.at[color, 1]).wait_send()
    amount(columns_in, p_send, p_recv).wait_send()
    amount(rows_in, d_send, d_recv).wait_send()
    amount(rows_in, c_send, c_recv).wait_send()


def leave_kernel(result_ref, state_ref, result_hbm, state_hbm, sem):
    copies = [
        pltpu.make_async_copy(state_ref, state_hbm, sem.at[0]),
        pltpu.make_async_copy(result_ref, result_hbm, sem.at[1]),
    ]
    for copy in copies:
        copy.start()
    for copy in copies:
        copy.wait()


def shards(
    residual_in,
    gain_mix_pre,
    w_query,
    w_key,
    w_value,
    w_outgate,
    w_decay,
    w_beta,
    decay_scale,
    decay_bias,
    head_gain,
    w_out,
    gain_mix_post,
    state_cache,
    gain_ffn_pre,
    routes,
    route_logits,
    w_gate,
    w_up,
    w_down,
    gain_ffn_post,
):
    vmem = pl.BlockSpec(memory_space=pltpu.VMEM)
    hbm = pl.BlockSpec(memory_space=pl.ANY)
    dma = pltpu.SemaphoreType.DMA

    def row(vector):
        return vector.reshape(1, -1)

    head_rows = pltpu.VMEM((H, 8, HD), F32)
    result, new_state = pl.pallas_call(
        layer_kernel,
        out_shape=(
            jax.ShapeDtypeStruct((8, D), BF),
            jax.ShapeDtypeStruct((8, H, HD, HD), BF),
        ),
        in_specs=[vmem] * 12 + [hbm] * 9,
        out_specs=(vmem, vmem),
        scratch_shapes=[
            pltpu.VMEM((128, D), BF),
            pltpu.VMEM((4, 4, 4, 8, D), BF),
            pltpu.VMEM((4, 4, 4, 8, 128), F32),
            pltpu.VMEM((4, 4, 4, 8, 128), BF),
            pltpu.VMEM((4, 4, 4, 8, 128), BF),
            head_rows,
            head_rows,
            head_rows,
            head_rows,
            head_rows,
            head_rows,
            head_rows,
            head_rows,
            pltpu.VMEM((8, H, HD, HD), BF),
            pltpu.VMEM((D, D), BF),
            pltpu.VMEM((D, 1024), BF),
            pltpu.VMEM((D, 1024), BF),
            pltpu.VMEM((1024, D), BF),
            pltpu.VMEM((8, D), F32),
            pltpu.VMEM((64, D), BF),
            pltpu.VMEM((128, D), BF),
            pltpu.VMEM((128, 1024), BF),
            pltpu.VMEM((128, D), BF),
            pltpu.VMEM((128, D), BF),
            dma((9,)),
            dma((7,)),
            dma((7,)),
            dma((3,)),
            dma((3, 4)),
            dma((3,)),
            dma((3, 4)),
            dma(()),
            dma(()),
            dma(()),
            dma(()),
            dma(()),
            dma(()),
        ],
        compiler_params=pltpu.CompilerParams(
            collective_id=0, has_side_effects=True, vmem_limit_bytes=56 * 1024 * 1024
        ),
    )(
        residual_in,
        row(gain_mix_pre),
        w_decay.T,
        w_beta.T,
        row(decay_scale),
        row(decay_bias),
        row(head_gain),
        row(gain_mix_post),
        row(gain_ffn_pre),
        routes.T,
        route_logits.T,
        row(gain_ffn_post),
        w_query.T,
        w_key.T,
        w_value.T,
        w_outgate.T,
        w_out,
        state_cache,
        w_gate,
        w_up,
        w_down,
    )
    return pl.pallas_call(
        leave_kernel,
        out_shape=(
            jax.ShapeDtypeStruct((8, D), BF),
            jax.ShapeDtypeStruct((8, H, HD, HD), BF),
        ),
        in_specs=[vmem, vmem],
        out_specs=(hbm, hbm),
        scratch_shapes=[dma((2,))],
    )(result, new_state)


def solution(mesh):
    in_specs = (
        P("ep", None),
        P(),
        P(None, "ep"),
        P(None, "ep"),
        P(None, "ep"),
        P(None, "ep"),
        P(),
        P(),
        P(),
        P(),
        P(),
        P(),
        P(),
        P("ep", None, None, None),
        P(),
        P("ep", None),
        P("ep", None),
        P(None, "ep"),
        P(None, "ep"),
        P("ep", None),
        P(),
    )
    out_specs = (P("ep", None), P("ep", None, None, None))
    return jax.shard_map(shards, mesh=mesh, in_specs=in_specs, out_specs=out_specs, check_vma=False)
```
